32 devices in a mesh: rep: 2 (over y), fs: 4 (over z), tp: 4 (over x, core).
Axes of the slice: x: 2, y: 2, z: 4, core: 2. Of those that a mesh axis runs over, the one named last changes fastest.
Arguments:
- out_grad: bfloat16 [2048, 2048], P(('rep', 'fs'), 'tp'), may hold values from -6 to 6
- gate_lin: bfloat16 [2048, 5632], P(('rep', 'fs'), 'tp'), may hold values from -6 to 6
- up_lin: bfloat16 [2048, 5632], P(('rep', 'fs'), 'tp'), may hold values from -6 to 6
- conv_weight: bfloat16 [3, 5632], replicated, may hold values from -3.5 to 3.5
- gate_weight: bfloat16 [2048, 5632], P('fs', 'tp'), may hold values from -0.125 to 0.125
- up_weight: bfloat16 [2048, 5632], P('fs', 'tp'), may hold values from -0.125 to 0.125
- down_weight: bfloat16 [5632, 2048], P('tp', 'fs'), may hold values from -0.078125 to 0.078125
Outputs:
- input_grad: bfloat16 [2048, 2048], P(('rep', 'fs'), 'tp')
- conv_grad: float32 [3, 5632], replicated
The draws below stay inside these ranges and needn't reach their ends.
All inputs are finite; a program needn't handle non-finite values.
Results may differ from the reference program's by a relative error of at most 0.015.
Values may be sent and summed in bfloat16 or wider, within the bound.
A program may use at most 64 MiB of HBM per device.

```python
import math
from functools import partial
import jax
import jax.numpy as jnp
from jax import lax

D = 2048
FF = 5632
SEQ = 1024
SEQS = 2
TOKENS = 2048
N_TP = 4


def strengthened(entries, key, source, target, parts, factor):
    owner, partner = [(jnp.arange(entries.shape[axis_at]) // (entries.shape[axis_at] // parts)).reshape([-1 if axis == axis_at else 1 for axis in range(entries.ndim)]) for axis_at in (source, target)]
    chosen = jax.random.permutation(key, parts)[partner]
    strong = (owner == chosen) | (owner == (partner + parts // 2) % parts)
    return jnp.where(strong, factor * entries, entries)


def levels(own_key, extent, split, smallest, high):
    loudness, own = 1.0, jax.random.fold_in(own_key, 6)
    for axis_at, blocks in split:
        steps = jnp.exp(jax.random.uniform(jax.random.fold_in(own, axis_at), (blocks,), jnp.float32, smallest / len(split), high / len(split)))
        loudness = loudness * jnp.repeat(steps, extent[axis_at] // blocks).reshape([-1 if axis == axis_at else 1 for axis in range(len(extent))])
    return loudness


def bell_draw(own_key, dims, spread, limit, cuts=(), dtype=jnp.bfloat16):
    array = spread * jax.random.normal(own_key, dims, jnp.float32)
    if cuts:
        array = array * levels(own_key, dims, cuts, -0.22, 0.18)
    return jnp.clip(array, -limit, limit).astype(dtype)


def gaussian_with(stream_key, extent, width, bound, split, heavy, dtype=jnp.bfloat16):
    result = width * jax.random.normal(stream_key, extent, jnp.float32)
    if split:
        result = result * levels(stream_key, extent, split, -0.22, 0.18)
    return jnp.clip(strengthened(result, jax.random.fold_in(stream_key, 3), *heavy), -bound, bound).astype(dtype)


def setup_inputs(seed: int = 0) -> dict:
    streams_of = jax.random.split(jax.random.key(seed), 8)
    return {
        "out_grad": gaussian_with(streams_of[0], (TOKENS, D), 1.0, 6.0, ((0, 8), (1, 4)), (0, 1, 8, 2.0)),
        "gate_lin": bell_draw(streams_of[1], (TOKENS, FF), 1.0, 6.0, ((0, 8), (1, 4))),
        "up_lin": bell_draw(streams_of[2], (TOKENS, FF), 1.0, 6.0, ((0, 8), (1, 4))),
        "conv_weight": bell_draw(streams_of[3], (3, FF), 3 ** -0.5, 3.5),
        "gate_weight": bell_draw(streams_of[4], (D, FF), D ** -0.5, 0.125, ((0, 4), (1, 4))),
        "up_weight": bell_draw(streams_of[5], (D, FF), D ** -0.5, 0.125, ((0, 4), (1, 4))),
        "down_weight": bell_draw(streams_of[6], (FF, D), FF ** -0.5, 0.078125, ((0, 4), (1, 4))),
    }


def gelu_parts(gate):
    normal_cdf = 0.5 * (1.0 + jax.scipy.special.erf(gate * (1.0 / math.sqrt(2.0))))
    density = jnp.exp(-0.5 * gate * gate) * (1.0 / math.sqrt(2.0 * math.pi))
    return (gate * normal_cdf, normal_cdf + gate * density)

def shifted(values):
    zero_row = jnp.zeros_like(values[:1])
    before = jnp.concatenate([zero_row, values[:-1]], axis=0)
    after = jnp.concatenate([values[1:], zero_row], axis=0)
    return (before, after)

def one_sequence(packed, conv_weight, gate_weight, up_weight, down_weight):
    grad_block, gate_block, up_block = packed
    conv_taps = conv_weight.astype(jnp.float32)
    linear = gate_block.astype(jnp.float32)
    before, after = shifted(linear)
    gate = conv_taps[0] * before + conv_taps[1] * linear + conv_taps[2] * after
    gelu_value, gelu_slope = gelu_parts(gate)
    act_grad = jnp.dot(grad_block, down_weight.T, preferred_element_type=jnp.float32)
    gate_grad = act_grad * up_block.astype(jnp.float32) * gelu_slope
    up_grad = (act_grad * gelu_value).astype(jnp.bfloat16)
    grad_before, grad_after = shifted(gate_grad)
    linear_grad = (conv_taps[0] * grad_after + conv_taps[1] * gate_grad + conv_taps[2] * grad_before).astype(jnp.bfloat16)
    conv_grad = jnp.stack([lax.optimization_barrier(jnp.sum(gate_grad * before, axis=0)), lax.optimization_barrier(jnp.sum(gate_grad * linear, axis=0)), lax.optimization_barrier(jnp.sum(gate_grad * after, axis=0))])
    block_width = FF // N_TP
    summed = jnp.zeros((grad_block.shape[0], D), jnp.float32)
    for block_index in range(N_TP):
        column_low = block_index * block_width
        column_high = column_low + block_width
        partial_sum = jnp.dot(linear_grad[:, column_low:column_high], gate_weight[:, column_low:column_high].T, preferred_element_type=jnp.float32)
        partial_sum = partial_sum + jnp.dot(up_grad[:, column_low:column_high], up_weight[:, column_low:column_high].T, preferred_element_type=jnp.float32)
        rounded = lax.optimization_barrier(partial_sum.astype(jnp.bfloat16))
        summed = summed + rounded.astype(jnp.float32)
    return (summed.astype(jnp.bfloat16), conv_grad)

def reference(out_grad, gate_lin, up_lin, conv_weight, gate_weight, up_weight, down_weight):
    grads = out_grad.reshape(SEQS, SEQ, D)
    gates = gate_lin.reshape(SEQS, SEQ, FF)
    ups = up_lin.reshape(SEQS, SEQ, FF)
    worker = partial(one_sequence, conv_weight=conv_weight, gate_weight=gate_weight, up_weight=up_weight, down_weight=down_weight)
    input_blocks, conv_parts = lax.map(worker, (grads, gates, ups))
    return (input_blocks.reshape(TOKENS, D), lax.optimization_barrier(jnp.sum(conv_parts, axis=0)))
```

```python
import math

import jax
import jax.numpy as jnp
from jax import lax
from jax.sharding import PartitionSpec as P


def extended(value, sides, width):
    for axis, dim in sides:
        peers, length = (lax.axis_size(axis), value.shape[dim])
        up = [(i, (i + 1) % peers) for i in range(peers - 1)]
        down = [(j, i) for i, j in up]
        last = lax.slice_in_dim(value, length - width, length, axis=dim)
        leading = lax.slice_in_dim(value, 0, width, axis=dim)
        before = lax.ppermute(last, axis, up)
        after = lax.ppermute(leading, axis, down)
        value = jnp.concatenate([before, value, after], axis=dim)
    return value


def gelu_parts(gate):
    normal_cdf = 0.5 * (1.0 + jax.scipy.special.erf(gate * (1.0 / math.sqrt(2.0))))
    density = jnp.exp(-0.5 * gate * gate) * (1.0 / math.sqrt(2.0 * math.pi))
    return (gate * normal_cdf, normal_cdf + gate * density)


def local(out_grad, gate_lin, up_lin, conv_weight, gate_weight, up_weight, down_weight):
    conv_full = conv_weight.astype(jnp.float32)
    column_count = gate_lin.shape[1]
    column_start = lax.axis_index("tp") * column_count
    conv_taps = lax.dynamic_slice_in_dim(conv_full, column_start, column_count, 1)
    grad_rows = lax.all_gather(out_grad, "tp", axis=1, tiled=True)
    act_grad = lax.dot_general(
        grad_rows,
        lax.all_gather(down_weight, "fs", axis=1, tiled=True),
        (((1,), (1,)), ((), ())),
        preferred_element_type=jnp.float32,
    )
    linear_mid = extended(gate_lin, (("fs", 0),), 1).astype(jnp.float32)
    gate = (
        conv_taps[0] * linear_mid[:-2]
        + conv_taps[1] * linear_mid[1:-1]
        + conv_taps[2] * linear_mid[2:]
    )
    gelu_value, gelu_slope = gelu_parts(gate)
    gate_grad = act_grad * up_lin.astype(jnp.float32) * gelu_slope
    grad_ext = extended(gate_grad.astype(jnp.bfloat16), (("fs", 0),), 1).astype(gate_grad.dtype)
    up_grad = (act_grad * gelu_value).astype(jnp.bfloat16)
    own_grad = grad_ext[1:-1]
    linear_grad = (
        conv_taps[0] * grad_ext[2:] + conv_taps[1] * own_grad + conv_taps[2] * grad_ext[:-2]
    ).astype(jnp.bfloat16)
    local_conv = jnp.stack(
        [
            jnp.sum(own_grad * linear_mid[:-2], axis=0),
            jnp.sum(own_grad * linear_mid[1:-1], axis=0),
            jnp.sum(own_grad * linear_mid[2:], axis=0),
        ]
    )
    product = lax.dot_general(
        linear_grad,
        lax.all_gather(gate_weight, "fs", axis=0, tiled=True),
        (((1,), (1,)), ((), ())),
        preferred_element_type=jnp.float32,
    )
    product = product + lax.dot_general(
        up_grad,
        lax.all_gather(up_weight, "fs", axis=0, tiled=True),
        (((1,), (1,)), ((), ())),
        preferred_element_type=jnp.float32,
    )
    input_grad = lax.psum_scatter(
        product.astype(jnp.bfloat16), "tp", scatter_dimension=1, tiled=True
    )
    summed_conv = lax.psum(local_conv, ("rep", "fs"))
    conv_grad = lax.all_gather(summed_conv, "tp", axis=1, tiled=True)
    return (input_grad, conv_grad)


def swap(value, axis, bit):
    size = lax.axis_size(axis)
    return lax.ppermute(value, axis, [(i, i ^ bit) for i in range(size)])


def after(value, *others):
    return lax.optimization_barrier((value, *others))[0]


def rows_dot(a, b):
    return lax.dot_general(a, b, (((1,), (1,)), ((), ())), preferred_element_type=jnp.float32)


def paired(out_grad, gate_lin, up_lin, conv_weight, gate_weight, up_weight, down_weight):
    f32, bf16 = jnp.float32, jnp.bfloat16
    rep, fs, tp = (lax.axis_index(a) for a in ("rep", "fs", "tp"))
    n_fs = lax.axis_size("fs")
    columns = gate_lin.shape[1]
    width = down_weight.shape[1]
    half = width // 2
    conv_taps = lax.dynamic_slice_in_dim(conv_weight, tp * columns, columns, 1).astype(f32)

    def rep_swap(value, places):
        perm = [(r * n_fs + p, (1 - r) * n_fs + p) for r in range(2) for p in places]
        return lax.ppermute(value, ("rep", "fs"), perm)

    own_half = lax.dynamic_slice_in_dim(down_weight, rep * half, half, 1)
    r1 = lax.ppermute(own_half, "fs", [(0, 1), (1, 2), (2, 3)])
    l1 = lax.ppermute(own_half, "fs", [(1, 0), (2, 1), (3, 2)])
    r2 = lax.ppermute(r1, "fs", [(1, 2), (2, 3)])
    l2 = lax.ppermute(l1, "fs", [(1, 0), (2, 1)])
    c3 = lax.ppermute(jnp.where(fs == 2, r2, l2), "fs", [(2, 3), (1, 0)])

    pair = jnp.stack([out_grad, swap(out_grad, "tp", 2)])
    other = swap(pair, "tp", 1)
    blocks = jnp.stack([pair[0], other[0], pair[1], other[1]])
    rows = out_grad.shape[0]
    og = blocks.reshape(n_fs, rows, 2, half).transpose(0, 2, 1, 3).reshape(2 * n_fs, rows, half)

    def feature_half(block, part):
        block = jnp.clip(block, 0, n_fs - 1)
        return lax.dynamic_index_in_dim(og, (tp ^ block) * 2 + part, 0, keepdims=False)

    linear_mid = extended(gate_lin, (("fs", 0),), 1).astype(f32)
    gate = (
        conv_taps[0] * linear_mid[:-2]
        + conv_taps[1] * linear_mid[1:-1]
        + conv_taps[2] * linear_mid[2:]
    )

    act_grad = rows_dot(lax.dynamic_index_in_dim(blocks, tp ^ fs, 0, keepdims=False), down_weight)
    steps = (
        (r1, fs - 1, (1, 2, 3)),
        (l1, fs + 1, (0, 1, 2)),
        (r2, fs - 2, (2, 3)),
        (l2, fs + 2, (0, 1)),
        (c3, n_fs - 1 - fs, (0, 3)),
    )
    for piece, block, places in steps:
        second = rep_swap(piece, places)
        act_grad = act_grad + rows_dot(feature_half(block, rep), piece)
        act_grad = act_grad + rows_dot(feature_half(block, 1 - rep), second)

    def fetch(weight, *order):
        piece = lax.dynamic_slice_in_dim(weight, rep * half, half, 0)
        piece = swap(after(piece, *order), "fs", 2)
        return piece, swap(piece, "rep", 1)

    up_a, up_b = fetch(up_weight, r2, l2)
    gate_a, gate_b = fetch(gate_weight, up_a)

    gelu_value, gelu_slope = gelu_parts(gate)
    up_grad = (act_grad * gelu_value).astype(bf16)
    up_far = swap(up_grad, "fs", 1)
    gate_grad = act_grad * up_lin.astype(f32) * gelu_slope
    grad_ext = extended(gate_grad.astype(bf16), (("fs", 0),), 1).astype(f32)
    linear_grad = (
        conv_taps[0] * grad_ext[2:] + conv_taps[1] * gate_grad + conv_taps[2] * grad_ext[:-2]
    ).astype(bf16)
    linear_far = swap(linear_grad, "fs", 1)

    conv_grad = jnp.stack(
        [
            jnp.sum(gate_grad * linear_mid[:-2], axis=0),
            jnp.sum(gate_grad * linear_mid[1:-1], axis=0),
            jnp.sum(gate_grad * linear_mid[2:], axis=0),
        ]
    )
    for axis, bit in (("fs", 1), ("fs", 2), ("rep", 1)):
        conv_grad = conv_grad + swap(conv_grad, axis, bit)
    for bit in (1, 2):
        far = swap(conv_grad, "tp", bit)
        low = (tp & bit) == 0
        conv_grad = jnp.where(
            low,
            jnp.concatenate([conv_grad, far], axis=1),
            jnp.concatenate([far, conv_grad], axis=1),
        )

    def product(linear, up):
        near = rows_dot(up, up_weight) + rows_dot(linear, gate_weight)
        a = rows_dot(up, up_a) + rows_dot(linear, gate_a)
        b = rows_dot(up, up_b) + rows_dot(linear, gate_b)
        far = jnp.where(
            rep == 0, jnp.concatenate([a, b], axis=1), jnp.concatenate([b, a], axis=1)
        )
        return near.astype(bf16), far.astype(bf16)

    own0, own2 = product(linear_grad, up_grad)
    far0, far2 = product(linear_far, up_far)
    parts = jnp.stack([own0, far0, own2, far2])

    def part(member):
        return lax.dynamic_index_in_dim(parts, member ^ fs, 0, keepdims=False)

    sent = jnp.stack([part(tp ^ 1), part(tp ^ 3)])
    got = swap(sent, "tp", 1).astype(f32)
    mine = part(tp).astype(f32) + got[0]
    theirs = (part(tp ^ 2).astype(f32) + got[1]).astype(bf16)
    summed = (mine + swap(theirs, "tp", 2).astype(f32)).astype(bf16)
    n_tp = lax.axis_size("tp")
    crossing = [
        (p * n_tp + q, (p ^ 1) * n_tp + (q ^ 1))
        for p in range(n_fs)
        for q in range(n_tp)
        if ((p ^ q) & 1) == 1
    ]
    crossed = lax.ppermute(summed, ("fs", "tp"), crossing)
    input_grad = jnp.where(((fs ^ tp) & 1) == 1, crossed, summed)
    return (input_grad, conv_grad)


def solution(mesh):
    sizes = tuple(mesh.shape[a] for a in ("rep", "fs", "tp"))
    return jax.shard_map(
        paired if sizes == (2, 4, 4) else local,
        mesh=mesh,
        in_specs=(
            P(("rep", "fs"), "tp"),
            P(("rep", "fs"), "tp"),
            P(("rep", "fs"), "tp"),
            P(),
            P("fs", "tp"),
            P("fs", "tp"),
            P("tp", "fs"),
        ),
        out_specs=(P(("rep", "fs"), "tp"), P()),
        check_vma=False,
    )
```
